32 devices in a mesh: sp: 8 (over z, x), tp: 4 (over y, core).
Axes of the slice: x: 2, y: 2, z: 4, core: 2. Of those that a mesh axis runs over, the one named last changes fastest.
Arguments:
- queries: bfloat16 [2048, 1024], P('sp', 'tp'), may hold values from -6 to 6
- keys: bfloat16 [2048, 256], P('sp'), may hold values from -6 to 6
- values: bfloat16 [2048, 256], P('sp'), may hold values from -6 to 6
- sink: float32 [16], P('tp'), may hold values from 3 to 6
- w_out: bfloat16 [1024, 2048], P('tp'), may hold values from -0.1875 to 0.1875
- stream: bfloat16 [2048, 2048], P(('sp', 'tp')), may hold values from -6 to 6
- gain: bfloat16 [2048], replicated, may hold values from 0.099609375 to 1.8984375
- routes: int32 [2048, 4], P('sp'), may hold values from 0 to 63, all different within a row; in each aligned block of 64 rows (0 to 63, 64 to 127, ...) at most 8 rows name the same one
- route_weights: float32 [2048, 4], P('sp'), may hold values from 0.2 to 1
- w_gate: bfloat16 [64, 1024, 2048], P('sp', 'tp'), may hold values from -0.125 to 0.125
- w_up: bfloat16 [64, 1024, 2048], P('sp', 'tp'), may hold values from -0.125 to 0.125
- w_down: bfloat16 [64, 1024, 2048], P('sp', None, 'tp'), may hold values from -0.1875 to 0.1875
- shared_gate: bfloat16 [1024, 2048], P('tp'), may hold values from -0.125 to 0.125
- shared_up: bfloat16 [1024, 2048], P('tp'), may hold values from -0.125 to 0.125
- shared_down: bfloat16 [1024, 2048], P(None, 'tp'), may hold values from -0.1875 to 0.1875
Outputs:
- layer_out: bfloat16 [2048, 2048], P('sp', 'tp')
The draws below stay inside these ranges and needn't reach their ends.
Inputs may be any that keep to these rules, and one draw needn't show every extreme that they name: `routes`: in each aligned block of 64 rows no expert is named in more than 8 rows, and some blocks reach 8; a row names 4 different experts.
All inputs are finite; a program needn't handle non-finite values.
Results may differ from the reference program's by a relative error of at most 0.014.
Values may be sent and summed in bfloat16 or wider, within the bound.
A program may use at most 128 MiB of HBM per device.

```python
import math
import jax
import jax.numpy as jnp
import numpy as np
from jax import lax

D = 2048
HEADS = 16
KV_HEADS = 4
HD = 64
WINDOW = 128
EXPERTS = 64
TOPK = 4
FE = 1024
FS = 1024
TOKENS = 2048
ROWS_DEV = 64
CAP = 8
N_SP = 8
N_TP = 4


def draw_queries(key, part):
    base_key = jax.random.fold_in(key, 1)
    base_draw = jax.random.truncated_normal(base_key, -6.0, 6.0, (TOKENS, HEADS, HD), jnp.float32)
    return base_draw.reshape(TOKENS, HEADS * HD).astype(jnp.bfloat16)


def draw_keys(key, part):
    base_key = jax.random.fold_in(key, 2)
    base_draw = jax.random.truncated_normal(base_key, -6.0, 6.0, (TOKENS, KV_HEADS, HD), jnp.float32)
    return base_draw.reshape(TOKENS, KV_HEADS * HD).astype(jnp.bfloat16)


def block_levels(stream_key, extent, pieces, smallest, high):
    def one(dim, blocks):
        heights = jax.random.uniform(jax.random.fold_in(jax.random.fold_in(stream_key, 6), dim), (blocks,), jnp.float32, smallest / len(pieces), high / len(pieces))
        return jnp.repeat(jnp.exp(heights), extent[dim] // blocks).reshape((-1,) + (1,) * (len(extent) - dim - 1))

    factor_of = one(*pieces[0])
    for cut in pieces[1:]:
        factor_of = factor_of * one(*cut)
    return factor_of


def deal_out(stream_key, own, number, rows, amount, top, reach, lean):
    order = jax.random.permutation(stream_key, amount)
    packed, usual = portions_of(amount, rows * top, reach, lean, True), portions_of(amount, rows * top, reach, lean, False)
    places = jnp.arange(amount)

    def named(sizes, rotation):
        used = int((sizes > 0).sum())
        fixed = max(1, used // 4)
        passed = fixed + (places - fixed + rotation * (used - fixed)) % max(1, amount - fixed)
        return jnp.zeros((amount,), jnp.int32).at[order[jnp.where(places < fixed, places, passed)]].set(jnp.asarray(sizes, jnp.int32))

    sizes = jnp.where(number % 4 == 0, named(packed, number // 4), named(usual, number - number // 4 - 1))
    mixed = jax.random.permutation(jax.random.fold_in(own, 3), amount)
    giver, taker = mixed[0:amount // 2 * 2:2], mixed[1:amount // 2 * 2:2]
    room = jnp.minimum(sizes[giver] - 1, reach - sizes[taker]) // 2
    room = jnp.where((giver == order[0]) | (taker == order[0]) | (sizes[taker] == 0), 0, jnp.maximum(room, 0))
    passed = jax.random.randint(jax.random.fold_in(own, 4), (amount // 2,), 0, 1 << 20) % (room + 1)
    sizes = sizes.at[giver].add(-passed).at[taker].add(passed)
    items = jnp.searchsorted(jnp.cumsum(sizes), jnp.arange(rows * top), side="right").astype(jnp.int32)
    grid = items.reshape(top, rows).T
    grid = grid[jax.random.permutation(jax.random.fold_in(own, 1), rows)]
    rotation = jax.random.randint(jax.random.fold_in(own, 2), (rows, 1), 0, top)
    return jnp.take_along_axis(grid, (jnp.arange(top)[None, :] + rotation) % top, axis=1)


def portions_of(amount, total, bound, skew, full):
    portions = [(1 << 20) // math.isqrt(grade ** skew) + 1 for grade in range(1, amount + 1)]
    largest = bound if full else min(bound, max(-(-total // amount), total * portions[0] // sum(portions)))
    least = 1 if total - largest >= amount - 1 else 0
    given, surplus = [largest] + [least] * (amount - 1), total - largest - least * (amount - 1)
    while surplus > 0:
        candidates = [i for i in range(1, amount) if given[i] < largest] or [i for i in range(1, amount) if given[i] < bound]
        mass, left = sum([portions[i] for i in candidates]), surplus
        for i in candidates:
            addition = min(bound - given[i], max(1, left * portions[i] // mass), surplus)
            given[i] = given[i] + addition
            surplus = surplus - addition
    return np.array(given)


def bell_draw(rng, dims, scale, reach, cuts=(), dtype=jnp.bfloat16):
    level = block_levels(rng, dims, cuts, -0.22, 0.18) if cuts else 1.0
    result = jax.random.normal(rng, dims, jnp.float32) * scale * level
    return jnp.minimum(jnp.maximum(result, -reach), reach).astype(dtype)


def setup_inputs(seed: int = 0) -> dict:
    arg_keys = jax.random.split(jax.random.key(seed), 16)
    queries = draw_queries(jax.random.fold_in(arg_keys[15], 71), 0)
    keys = draw_keys(jax.random.fold_in(arg_keys[15], 71), 0)
    values = bell_draw(arg_keys[2], (TOKENS, KV_HEADS * HD), 1.0, 6.0, ((0, 8),))
    sink = jnp.clip(3.0 + 3.0 * jax.random.uniform(arg_keys[3], (HEADS,), jnp.float32) ** block_levels(arg_keys[3], (HEADS,), ((0, 4),), -0.2, 0.2), 3.0, 6.0)
    w_out = bell_draw(arg_keys[4], (HEADS * HD, D), (HEADS * HD) ** -0.5, 0.1875, ((0, 4),))
    stream = bell_draw(arg_keys[5], (TOKENS, D), 1.0, 6.0, ((0, 32),))
    gain = jnp.clip(1.0 + 0.18 * jax.random.normal(arg_keys[6], (D,), jnp.float32), 0.099609375, 1.8984375).astype(jnp.bfloat16)
    routes_keys = jax.random.split(jax.random.fold_in(arg_keys[7], 1), TOKENS // ROWS_DEV)
    routes_turns = jax.random.permutation(jax.random.fold_in(arg_keys[7], 3), TOKENS // ROWS_DEV)
    routes = jax.vmap(lambda own, number: deal_out(jax.random.fold_in(arg_keys[7], 2), own, number, ROWS_DEV, EXPERTS, TOPK, CAP, 2))(routes_keys, routes_turns).reshape((TOKENS, TOPK))
    route_weights = jnp.clip(0.2 + 0.8 * jax.random.uniform(arg_keys[8], (TOKENS, TOPK), jnp.float32) ** block_levels(arg_keys[8], (TOKENS, TOPK), ((0, 8),), -0.2, 0.2), 0.2, 1.0)
    w_gate = bell_draw(arg_keys[9], (EXPERTS, FE, D), D ** -0.5, 0.125, ((0, 8), (1, 4)))
    w_up = bell_draw(arg_keys[10], (EXPERTS, FE, D), D ** -0.5, 0.125, ((0, 8), (1, 4)))
    w_down = bell_draw(arg_keys[11], (EXPERTS, FE, D), FE ** -0.5, 0.1875, ((0, 8), (2, 4)))
    shared_gate = bell_draw(arg_keys[12], (FS, D), D ** -0.5, 0.125, ((0, 4),))
    shared_up = bell_draw(arg_keys[13], (FS, D), D ** -0.5, 0.125, ((0, 4),))
    shared_down = bell_draw(arg_keys[14], (FS, D), FS ** -0.5, 0.1875, ((1, 4),))
    return dict(queries=queries, keys=keys, values=values, sink=sink, w_out=w_out, stream=stream, gain=gain, routes=routes, route_weights=route_weights, w_gate=w_gate, w_up=w_up, w_down=w_down, shared_gate=shared_gate, shared_up=shared_up, shared_down=shared_down)


NORM_EPS = 1e-05

def attention_part(queries, keys, values, sink):
    group = HEADS // KV_HEADS
    blocks = TOKENS // WINDOW
    query_heads = queries.astype(jnp.float32).reshape(blocks, WINDOW, KV_HEADS, group, HD)

    def banded(source):
        padded = jnp.pad(source.astype(jnp.float32).reshape(TOKENS, KV_HEADS, HD), ((WINDOW, WINDOW), (0, 0), (0, 0)))
        framed = padded.reshape(blocks + 2, WINDOW, KV_HEADS, HD)
        return jnp.concatenate([framed[:-2], framed[1:-1], framed[2:]], axis=1)
    key_band = banded(keys)
    value_band = banded(values)
    scores = jnp.einsum('nqkgd,njkd->nkgqj', query_heads, key_band, precision=lax.Precision.HIGHEST) * HD ** (-0.5)
    query_pos = jnp.arange(blocks)[:, None, None] * WINDOW + jnp.arange(WINDOW)[None, :, None]
    key_pos = jnp.arange(blocks)[:, None, None] * WINDOW - WINDOW + jnp.arange(3 * WINDOW)[None, None, :]
    allowed = (jnp.abs(query_pos - key_pos) <= WINDOW) & (key_pos >= 0) & (key_pos < TOKENS)
    scores = jnp.where(allowed[:, None, None], scores, -jnp.inf)
    sink_level = sink.astype(jnp.float32).reshape(1, KV_HEADS, group, 1, 1)
    row_peak = jnp.maximum(scores.max(-1, keepdims=True), sink_level)
    probabilities = jnp.exp(scores - row_peak)
    denominator = probabilities.sum(-1, keepdims=True) + jnp.exp(sink_level - row_peak)
    rounded = lax.optimization_barrier((probabilities / denominator).astype(jnp.bfloat16)).astype(jnp.float32)
    attended = jnp.einsum('nkgqj,njkd->nqkgd', rounded, value_band, precision=lax.Precision.HIGHEST)
    return attended.astype(jnp.bfloat16).reshape(TOKENS, HEADS * HD)

def routed_part(normed, routes, route_weights, w_gate, w_up, w_down):
    most_rows = N_SP * N_TP * CAP
    flat_routes = routes.reshape(-1).astype(jnp.int32)
    flat_weights = route_weights.reshape(-1).astype(jnp.float32)
    sorted_ids = jnp.argsort(flat_routes, stable=True).astype(jnp.int32)
    counts = lax.optimization_barrier(jnp.sum((flat_routes[:, None] == jnp.arange(EXPERTS)[None, :]).astype(jnp.int32), axis=0))
    starts = (jnp.cumsum(counts) - counts).astype(jnp.int32)
    padded = jnp.concatenate([sorted_ids, jnp.zeros((most_rows,), jnp.int32)])

    def one_expert(accumulated, expert):
        picked = lax.dynamic_slice(padded, (starts[expert].astype(jnp.int32),), (most_rows,))
        is_valid = jnp.arange(most_rows) < counts[expert]
        token_ids = (picked // TOPK).astype(jnp.int32)
        picked_rows = normed[token_ids]
        gate_act = jnp.dot(picked_rows, w_gate[expert].T, preferred_element_type=jnp.float32)
        up_act = jnp.dot(picked_rows, w_up[expert].T, preferred_element_type=jnp.float32)
        hidden = (jax.nn.silu(gate_act) * up_act).astype(jnp.bfloat16)
        expert_out = jnp.dot(hidden, w_down[expert], preferred_element_type=jnp.float32)
        expert_out = lax.optimization_barrier(expert_out.astype(jnp.bfloat16)).astype(jnp.float32)
        scale_col = jnp.where(is_valid, flat_weights[picked], 0.0).astype(jnp.float32)
        return (accumulated.at[token_ids].add(expert_out * scale_col[:, None]), None)
    total_init = jnp.zeros((TOKENS, D), jnp.float32)
    routed, unused = lax.scan(one_expert, total_init, jnp.arange(EXPERTS))
    return routed

def reference(queries, keys, values, sink, w_out, stream, gain, routes, route_weights, w_gate, w_up, w_down, shared_gate, shared_up, shared_down):
    attended = attention_part(queries, keys, values, sink)
    projected = jnp.dot(attended, w_out, preferred_element_type=jnp.float32)
    mixed_rows = (stream.astype(jnp.float32) + projected).astype(jnp.bfloat16)
    wide_rows = mixed_rows.astype(jnp.float32)
    scale_rows = lax.rsqrt(lax.optimization_barrier(jnp.mean(wide_rows * wide_rows, axis=-1, keepdims=True)) + NORM_EPS)
    normed = (wide_rows * scale_rows * gain.astype(jnp.float32)).astype(jnp.bfloat16)
    routed = routed_part(normed, routes, route_weights, w_gate, w_up, w_down)
    shared_gate_act = jnp.dot(normed, shared_gate.T, preferred_element_type=jnp.float32)
    shared_up_act = jnp.dot(normed, shared_up.T, preferred_element_type=jnp.float32)
    shared_hidden = (jax.nn.silu(shared_gate_act) * shared_up_act).astype(jnp.bfloat16)
    shared_out = jnp.dot(shared_hidden, shared_down, preferred_element_type=jnp.float32)
    return (wide_rows + routed + shared_out).astype(jnp.bfloat16)
```

```python
import functools

import jax
import jax.numpy as jnp
from jax import lax
from jax.experimental import pallas as pl
from jax.experimental.pallas import tpu as pltpu
from jax.sharding import PartitionSpec as P

D = 2048
HEADS = 16
KV_HEADS = 4
HD = 64
WINDOW = 128
EXPERTS = 64
TOPK = 4
NORM_EPS = 1e-05
CORES = 2
MOST_BLOCKS = 64
MESH = pl.DeviceIdType.MESH
ANY = pl.BlockSpec(memory_space=pl.ANY)
VMEM = pl.BlockSpec(memory_space=pltpu.VMEM)


def greet(peers):
    barrier = pltpu.get_barrier_semaphore()
    for peer in peers:
        pl.semaphore_signal(barrier, inc=1, device_id=peer, device_id_type=MESH)
    pl.semaphore_wait(barrier, len(peers))


def remote(src, dst, send_sem, recv_sem, peer):
    return pltpu.make_async_remote_copy(
        src_ref=src,
        dst_ref=dst,
        send_sem=send_sem,
        recv_sem=recv_sem,
        device_id=peer,
        device_id_type=MESH,
    )


def grid_of(n_sp, n_tp):
    nx = 1
    while nx * nx * 4 <= n_sp and n_sp % (nx * 2) == 0:
        nx *= 2
    nc = CORES if n_tp % CORES == 0 else 1
    return n_sp // nx, nx, n_tp // nc, nc


def halo_kernel(n_sp, meta_ref, edges_ref, metas_ref, halo_ref, send_sem, recv_sem, edge_send, edge_recv):
    sp, tp = lax.axis_index("sp"), lax.axis_index("tp")
    greet([(lax.rem(sp + d, n_sp), tp) for d in range(1, n_sp)])
    copies = []
    for side, d in ((0, 1), (1, n_sp - 1)):
        copies.append(
            remote(
                edges_ref.at[side],
                halo_ref.at[side],
                edge_send.at[side],
                edge_recv.at[side],
                (lax.rem(sp + d, n_sp), tp),
            )
        )
    for d in range(1, n_sp):
        copies.append(
            remote(
                meta_ref,
                metas_ref.at[d],
                send_sem.at[d - 1],
                recv_sem.at[d - 1],
                (lax.rem(sp + d, n_sp), tp),
            )
        )
    for copy in copies:
        copy.start()
    metas_ref[0] = meta_ref[...]
    for copy in copies:
        copy.wait()


def exchange_halo(meta, edges, n_sp):
    return pl.pallas_call(
        functools.partial(halo_kernel, n_sp),
        out_shape=(
            jax.ShapeDtypeStruct((n_sp,) + meta.shape, meta.dtype),
            jax.ShapeDtypeStruct(edges.shape, edges.dtype),
        ),
        in_specs=[VMEM, VMEM],
        out_specs=(VMEM, VMEM),
        scratch_shapes=[
            pltpu.SemaphoreType.DMA((n_sp - 1,)),
            pltpu.SemaphoreType.DMA((n_sp - 1,)),
            pltpu.SemaphoreType.DMA((2,)),
            pltpu.SemaphoreType.DMA((2,)),
        ],
        compiler_params=pltpu.CompilerParams(collective_id=0, has_side_effects=True),
        name="halo",
    )(meta, edges)


def exchange_kernel(count, pieces, place, parts_ref, out_ref, send_sem, recv_sem):
    me, peer_at = place()
    greet([peer_at(lax.rem(me + d, count)) for d in range(1, count)])
    copies = []
    for piece in range(pieces):
        for d in range(1, count):
            there = lax.rem(me + d, count)
            copies.append(
                remote(
                    parts_ref.at[there, piece],
                    out_ref.at[d - 1, piece],
                    send_sem.at[d - 1, piece],
                    recv_sem.at[d - 1, piece],
                    peer_at(there),
                )
            )
    for copy in copies:
        copy.start()
    for copy in copies:
        copy.wait()


def exchange(parts, count, place, collective_id, name):
    pieces = parts.shape[1]
    return pl.pallas_call(
        functools.partial(exchange_kernel, count, pieces, place),
        out_shape=jax.ShapeDtypeStruct((count - 1,) + parts.shape[1:], parts.dtype),
        in_specs=[ANY],
        out_specs=ANY,
        scratch_shapes=[
            pltpu.SemaphoreType.DMA((count - 1, pieces)),
            pltpu.SemaphoreType.DMA((count - 1, pieces)),
        ],
        compiler_params=pltpu.CompilerParams(
            collective_id=collective_id, has_side_effects=True
        ),
        name=name,
    )(parts)


def world_kernel(grid, own_ref, out_ref, send_sem, recv_sem, own_sem):
    nz, nx, ny, nc = grid
    sp, tp = lax.axis_index("sp"), lax.axis_index("tp")
    z, x, y, c = sp // nx, lax.rem(sp, nx), tp // nc, lax.rem(tp, nc)
    half = own_ref.shape[1] // 2

    def device(dz, dx, dy, dc):
        at_z, at_x = lax.rem(z + dz, nz), lax.rem(x + dx, nx)
        at_y, at_c = lax.rem(y + dy, ny), lax.rem(c + dc, nc)
        return at_z * nx + at_x, at_y * nc + at_c

    z_peers = [device(d, 0, 0, 0) for d in range(1, nz)]
    x_peers = [device(0, d, 0, 0) for d in range(1, nx)]
    y_peers = [device(0, 0, d, 0) for d in range(1, ny)]
    c_peers = [device(0, 0, 0, d) for d in range(1, nc)]
    greet(z_peers + x_peers + y_peers + c_peers)
    sent = []

    def block_of(place):
        at_sp, at_tp = device(*place)
        return at_sp * (ny * nc) + at_tp

    def view(place, h):
        return out_ref.at[block_of(place), :, pl.ds(h * half, half)]

    def push(place, h, peers):
        own = place == (0, 0, 0, 0)
        src = own_ref.at[:, pl.ds(h * half, half)] if own else view(place, h)
        for peer in peers:
            copy = remote(
                src,
                view(place, h),
                send_sem.at[len(sent)],
                recv_sem.at[block_of(place), h],
                peer,
            )
            copy.start()
            sent.append(copy)

    def arrived(place, h):
        remote(
            view(place, h),
            view(place, h),
            send_sem.at[0],
            recv_sem.at[block_of(place), h],
            (sp, tp),
        ).wait_recv()

    mine = (0, 0, 0, 0)
    keep = pltpu.make_async_copy(own_ref, out_ref.at[block_of(mine)], own_sem)
    for h in range(2):
        push(mine, h, z_peers)
    first, second = (x_peers, y_peers), (y_peers, x_peers)
    for h in range(2):
        push(mine, h, first[h])
        push(mine, h, second[h])
        push(mine, h, c_peers)
    keep.start()

    def level_one(dz):
        for h in range(2):
            if dz > 0:
                arrived((dz, 0, 0, 0), h)
                push((dz, 0, 0, 0), h, first[h])
                push((dz, 0, 0, 0), h, second[h])
                push((dz, 0, 0, 0), h, c_peers)

    def level_two(dz):
        for h in range(2):
            for d in range(1, (nx, ny)[h]):
                place = (dz, d, 0, 0) if h == 0 else (dz, 0, d, 0)
                arrived(place, h)
                push(place, h, second[h])
                push(place, h, c_peers)

    def level_three(dz):
        for h in range(2):
            for da in range((nx, ny)[h]):
                for db in range(1, (ny, nx)[h]):
                    place = (dz, da, db, 0) if h == 0 else (dz, db, da, 0)
                    arrived(place, h)
                    push(place, h, c_peers)

    for step in range(nz + 2):
        if step < nz:
            level_one(step)
        if 0 <= step - 1 < nz:
            level_two(step - 1)
        if 0 <= step - 2 < nz:
            level_three(step - 2)
    for dz in range(nz):
        for dx in range(nx):
            for dy in range(ny):
                for dc in range(1, nc):
                    for h in range(2):
                        arrived((dz, dx, dy, dc), h)
    for copy in sent:
        copy.wait_send()
    keep.wait()


def gather_world(own, n_sp, n_tp):
    grid = grid_of(n_sp, n_tp)
    blocks = n_sp * n_tp
    return pl.pallas_call(
        functools.partial(world_kernel, grid),
        out_shape=jax.ShapeDtypeStruct((blocks,) + own.shape, own.dtype),
        in_specs=[VMEM],
        out_specs=ANY,
        scratch_shapes=[
            pltpu.SemaphoreType.DMA((2 * blocks,)),
            pltpu.SemaphoreType.DMA((blocks, 2)),
            pltpu.SemaphoreType.DMA,
        ],
        compiler_params=pltpu.CompilerParams(collective_id=1, has_side_effects=True),
        name="world",
    )(own)


def columns_kernel(ny, nc, pieces, own_ref, out_ref, send_sem, recv_sem, own_sem):
    sp, tp = lax.axis_index("sp"), lax.axis_index("tp")
    y, c = tp // nc, lax.rem(tp, nc)
    rows, width = own_ref.shape
    step = rows // pieces

    def member(dy, dc):
        return lax.rem(y + dy, ny) * nc + lax.rem(c + dc, nc)

    y_peers = [(sp, member(d, 0)) for d in range(1, ny)]
    c_peers = [(sp, member(0, d)) for d in range(1, nc)]
    greet(y_peers + c_peers)
    sent = []

    def view(dy, dc, piece):
        start = pl.multiple_of(member(dy, dc) * width, width)
        return out_ref.at[pl.ds(piece * step, step), pl.ds(start, width)]

    def push(dy, piece, peers):
        src = own_ref.at[pl.ds(piece * step, step)] if dy == 0 else view(dy, 0, piece)
        for peer in peers:
            copy = remote(
                src,
                view(dy, 0, piece),
                send_sem.at[len(sent)],
                recv_sem.at[member(dy, 0), piece],
                peer,
            )
            copy.start()
            sent.append(copy)

    def arrived(dy, dc, piece):
        ref = view(dy, dc, piece)
        remote(
            ref, ref, send_sem.at[0], recv_sem.at[member(dy, dc), piece], (sp, tp)
        ).wait_recv()

    start = pl.multiple_of(tp * width, width)
    keep = pltpu.make_async_copy(own_ref, out_ref.at[:, pl.ds(start, width)], own_sem)
    keep.start()
    for piece in range(pieces):
        push(0, piece, y_peers)
    for piece in range(pieces):
        push(0, piece, c_peers)
    for piece in range(pieces):
        for dy in range(1, ny):
            arrived(dy, 0, piece)
            push(dy, piece, c_peers)
    for piece in range(pieces):
        for dy in range(ny):
            for dc in range(1, nc):
                arrived(dy, dc, piece)
    for copy in sent:
        copy.wait_send()
    keep.wait()


def gather_columns(own, n_sp, n_tp):
    rows, width = own.shape
    if width % 128 or n_sp * n_tp > MOST_BLOCKS:
        return lax.all_gather(own, "tp", axis=1, tiled=True)
    _, _, ny, nc = grid_of(n_sp, n_tp)
    pieces = 9 if rows % (9 * 16) == 0 else 1
    return pl.pallas_call(
        functools.partial(columns_kernel, ny, nc, pieces),
        out_shape=jax.ShapeDtypeStruct((rows, n_tp * width), own.dtype),
        in_specs=[VMEM],
        out_specs=ANY,
        scratch_shapes=[
            pltpu.SemaphoreType.DMA((n_tp * pieces,)),
            pltpu.SemaphoreType.DMA((n_tp, pieces)),
            pltpu.SemaphoreType.DMA,
        ],
        compiler_params=pltpu.CompilerParams(collective_id=2, has_side_effects=True),
        name="columns",
    )(own)


def attention(queries, band, sink, sp_idx, n_sp):
    tok_dev = queries.shape[0]
    blocks = tok_dev // WINDOW
    heads_dev = queries.shape[1] // HD
    framed = band.reshape(blocks + 2, WINDOW, 2 * HD)
    banded = jnp.concatenate([framed[:-2], framed[1:-1], framed[2:]], axis=1)
    key_band = banded[:, :, :HD]
    value_band = banded[:, :, HD:]
    query_blocks = queries.reshape(blocks, WINDOW, heads_dev, HD)
    scores = jnp.einsum(
        "nqhd,njd->nhqj", query_blocks, key_band, preferred_element_type=jnp.float32
    ) * HD ** (-0.5)
    offset = sp_idx * tok_dev
    seq_total = tok_dev * n_sp
    query_pos = (
        offset + jnp.arange(blocks)[:, None, None] * WINDOW + jnp.arange(WINDOW)[None, :, None]
    )
    key_pos = (
        offset
        - WINDOW
        + jnp.arange(blocks)[:, None, None] * WINDOW
        + jnp.arange(3 * WINDOW)[None, None, :]
    )
    allowed = (jnp.abs(query_pos - key_pos) <= WINDOW) & (key_pos >= 0) & (key_pos < seq_total)
    scores = jnp.where(allowed[:, None], scores, -jnp.inf)
    sink_level = sink.reshape(1, heads_dev, 1, 1)
    row_peak = jnp.maximum(scores.max(-1, keepdims=True), sink_level)
    probabilities = jnp.exp(scores - row_peak)
    denominator = probabilities.sum(-1, keepdims=True) + jnp.exp(sink_level - row_peak)
    weights = (probabilities / denominator).astype(jnp.bfloat16)
    attended = jnp.einsum("nhqj,njd->nqhd", weights, value_band, preferred_element_type=jnp.float32)
    return attended.astype(jnp.bfloat16).reshape(tok_dev, heads_dev * HD)


def norm(rows, gain):
    wide = rows.astype(jnp.float32)
    scale = lax.rsqrt(jnp.mean(wide * wide, axis=-1, keepdims=True) + NORM_EPS)
    return (wide * scale * gain.astype(jnp.float32)).astype(jnp.bfloat16)


def local(
    queries,
    keys,
    values,
    sink,
    w_out,
    stream,
    gain,
    routes,
    route_weights,
    w_gate,
    w_up,
    w_down,
    shared_gate,
    shared_up,
    shared_down,
):
    tok_dev = queries.shape[0]
    n_tp = lax.axis_size("tp")
    n_sp = lax.axis_size("sp")
    tp_idx = lax.axis_index("tp")
    sp_idx = lax.axis_index("sp")
    nz, nx, ny, nc = grid_of(n_sp, n_tp)
    z_idx, x_idx = sp_idx // nx, lax.rem(sp_idx, nx)
    heads_dev = HEADS // n_tp
    group = HEADS // KV_HEADS
    kv_head = tp_idx * heads_dev // group
    key_own = lax.dynamic_slice_in_dim(keys, kv_head * HD, HD, 1)
    value_own = lax.dynamic_slice_in_dim(values, kv_head * HD, HD, 1)
    paired = jnp.concatenate([key_own, value_own], axis=1)
    edges = jnp.stack([paired[-WINDOW:], paired[:WINDOW]])
    meta = jnp.concatenate([routes.astype(jnp.float32).T, route_weights.T], axis=0)
    metas, halo = exchange_halo(meta, edges, n_sp)
    band = jnp.concatenate([halo[0], paired, halo[1]], axis=0)
    attended = attention(queries, band, sink, sp_idx, n_sp)
    rows_dev = tok_dev // n_tp
    d_dev = w_down.shape[2]

    partial = jnp.dot(attended, w_out, preferred_element_type=jnp.float32)
    parts = partial.astype(jnp.bfloat16).reshape(n_tp, 1, rows_dev, D)
    theirs = exchange(
        parts,
        n_tp,
        lambda: (lax.axis_index("tp"), lambda there: (lax.axis_index("sp"), there)),
        3,
        "heads",
    )
    own_part = lax.dynamic_slice_in_dim(partial, tp_idx * rows_dev, rows_dev, 0)
    projected = own_part + jnp.sum(theirs[:, 0].astype(jnp.float32), axis=0)
    mixed_rows = (stream.astype(jnp.float32) + projected).astype(jnp.bfloat16)
    if n_sp * n_tp > MOST_BLOCKS:
        normed = lax.all_gather(norm(mixed_rows, gain), ("sp", "tp"), axis=0)
        own_blocks = lax.all_gather(mixed_rows, "tp", axis=0, tiled=True)
    else:
        world = gather_world(mixed_rows, n_sp, n_tp)
        normed = norm(world, gain)
        own_blocks = lax.dynamic_slice_in_dim(world, sp_idx * n_tp, n_tp, 0).reshape(tok_dev, D)
    residual = lax.dynamic_slice_in_dim(own_blocks, tp_idx * d_dev, d_dev, 1).astype(jnp.float32)
    own_normed = norm(own_blocks, gain)

    exp_dev = w_gate.shape[0]
    capacity = max(1, 2 * tok_dev * TOPK // (n_tp * EXPERTS))
    n_blocks = n_sp * n_tp
    order = lax.rem(sp_idx - jnp.arange(n_sp) + n_sp, n_sp)
    pick = (order[None, :] == jnp.arange(n_sp)[:, None]).astype(jnp.float32)
    metas = jnp.sum(pick[:, :, None, None] * metas[None], axis=1)
    metas = metas.reshape(n_sp, 2, TOPK, n_tp, rows_dev).transpose(1, 0, 3, 2, 4)
    named = metas[0].reshape(n_blocks, 1, TOPK, rows_dev)
    weight = metas[1].reshape(n_blocks, 1, TOPK, rows_dev)
    experts = (sp_idx * exp_dev + jnp.arange(exp_dev)).astype(jnp.float32)
    hit = (named == experts[None, :, None, None]).astype(jnp.float32)
    hit_any = jnp.sum(hit, axis=2)
    hit_weight = jnp.sum(hit * weight, axis=2)
    earlier = (jnp.arange(rows_dev)[:, None] < jnp.arange(rows_dev)[None, :]).astype(jnp.bfloat16)
    rank = jnp.einsum(
        "bej,jr->ber", hit_any.astype(jnp.bfloat16), earlier, preferred_element_type=jnp.float32
    )
    slots = jnp.arange(capacity).astype(jnp.float32)
    select = (rank[:, :, None, :] == slots[None, None, :, None]) * hit_any[:, :, None, :]
    slot_weight = jnp.sum(select * hit_weight[:, :, None, :], axis=-1)
    table = select.astype(jnp.bfloat16)

    arrived = jnp.einsum(
        "becr,brd->ebcd", table, normed, preferred_element_type=jnp.float32
    ).astype(jnp.bfloat16)
    arrived = arrived.reshape(exp_dev, n_blocks * capacity, D)
    gate_act = jnp.einsum("emd,efd->emf", arrived, w_gate, preferred_element_type=jnp.float32)
    up_act = jnp.einsum("emd,efd->emf", arrived, w_up, preferred_element_type=jnp.float32)
    hidden = (jax.nn.silu(gate_act) * up_act).astype(jnp.bfloat16)
    shared_gate_act = jnp.einsum(
        "td,fd->tf", own_normed, shared_gate, preferred_element_type=jnp.float32
    )
    shared_up_act = jnp.einsum(
        "td,fd->tf", own_normed, shared_up, preferred_element_type=jnp.float32
    )
    shared_hidden = (jax.nn.silu(shared_gate_act) * shared_up_act).astype(jnp.bfloat16)
    routed_rows = exp_dev * n_blocks * capacity
    width = hidden.shape[2]
    both = jnp.concatenate([hidden.reshape(routed_rows, width), shared_hidden], axis=0)
    both = gather_columns(both, n_sp, n_tp)
    expert_piece = both[:routed_rows].reshape(exp_dev, n_blocks * capacity, n_tp * width)
    routed_out = jnp.einsum(
        "emf,efd->emd", expert_piece, w_down, preferred_element_type=jnp.float32
    )
    scaled = routed_out.reshape(exp_dev, n_blocks, capacity, d_dev)
    scaled = scaled * slot_weight.transpose(1, 0, 2)[..., None]
    scaled = scaled.astype(jnp.bfloat16)
    sums = jnp.einsum("becr,ebcd->brd", table, scaled, preferred_element_type=jnp.float32)
    sums = sums.reshape(nz, nx, tok_dev, d_dev).transpose(1, 0, 2, 3)
    from_x = exchange(
        sums.astype(jnp.bfloat16),
        nx,
        lambda: (
            lax.rem(lax.axis_index("sp"), nx),
            lambda there: (
                lax.axis_index("sp") // nx * nx + there,
                lax.axis_index("tp"),
            ),
        ),
        4,
        "rows_x",
    )
    line = lax.dynamic_index_in_dim(sums, x_idx, 0, keepdims=False)
    line = line + jnp.sum(from_x.astype(jnp.float32), axis=0)
    from_z = exchange(
        line.astype(jnp.bfloat16).reshape(nz, 1, tok_dev, d_dev),
        nz,
        lambda: (
            lax.axis_index("sp") // nx,
            lambda there: (
                there * nx + lax.rem(lax.axis_index("sp"), nx),
                lax.axis_index("tp"),
            ),
        ),
        5,
        "rows_z",
    )
    routed = lax.dynamic_index_in_dim(line, z_idx, 0, keepdims=False)
    routed = routed + jnp.sum(from_z[:, 0].astype(jnp.float32), axis=0)
    shared_total = jnp.dot(both[routed_rows:], shared_down, preferred_element_type=jnp.float32)
    return (residual + routed + shared_total).astype(jnp.bfloat16)


def solution(mesh):
    placed = (
        P("sp", "tp"),
        P("sp", None),
        P("sp", None),
        P("tp"),
        P("tp", None),
        P(("sp", "tp"), None),
        P(),
        P("sp", None),
        P("sp", None),
        P("sp", "tp", None),
        P("sp", "tp", None),
        P("sp", None, "tp"),
        P("tp", None),
        P("tp", None),
        P(None, "tp"),
    )
    return jax.shard_map(
        local, mesh=mesh, in_specs=placed, out_specs=P("sp", "tp"), check_vma=False
    )
```

```python
import functools

import jax
import jax.numpy as jnp
from jax import lax
from jax.experimental import pallas as pl
from jax.experimental.pallas import tpu as pltpu
from jax.sharding import PartitionSpec as P

D = 2048
HEADS = 16
KV_HEADS = 4
HD = 64
WINDOW = 128
EXPERTS = 64
TOPK = 4
NORM_EPS = 1e-05
CORES = 2
MOST_BLOCKS = 64
MESH = pl.DeviceIdType.MESH
ANY = pl.BlockSpec(memory_space=pl.ANY)
VMEM = pl.BlockSpec(memory_space=pltpu.VMEM)


def greet(peers):
    barrier = pltpu.get_barrier_semaphore()
    for peer in peers:
        pl.semaphore_signal(barrier, inc=1, device_id=peer, device_id_type=MESH)
    pl.semaphore_wait(barrier, len(peers))


def remote(src, dst, send_sem, recv_sem, peer):
    return pltpu.make_async_remote_copy(
        src_ref=src,
        dst_ref=dst,
        send_sem=send_sem,
        recv_sem=recv_sem,
        device_id=peer,
        device_id_type=MESH,
    )


def grid_of(n_sp, n_tp):
    nx = 1
    while nx * nx * 4 <= n_sp and n_sp % (nx * 2) == 0:
        nx *= 2
    nc = CORES if n_tp % CORES == 0 else 1
    return n_sp // nx, nx, n_tp // nc, nc


def halo_kernel(n_sp, meta_ref, edges_ref, metas_ref, halo_ref, send_sem, recv_sem, edge_send, edge_recv):
    sp, tp = lax.axis_index("sp"), lax.axis_index("tp")
    greet([(lax.rem(sp + d, n_sp), tp) for d in range(1, n_sp)])
    copies = []
    for side, d in ((0, 1), (1, n_sp - 1)):
        copies.append(
            remote(
                edges_ref.at[side],
                halo_ref.at[side],
                edge_send.at[side],
                edge_recv.at[side],
                (lax.rem(sp + d, n_sp), tp),
            )
        )
    for d in range(1, n_sp):
        copies.append(
            remote(
                meta_ref,
                metas_ref.at[d],
                send_sem.at[d - 1],
                recv_sem.at[d - 1],
                (lax.rem(sp + d, n_sp), tp),
            )
        )
    for copy in copies:
        copy.start()
    metas_ref[0] = meta_ref[...]
    for copy in copies:
        copy.wait()


def exchange_halo(meta, edges, n_sp):
    return pl.pallas_call(
        functools.partial(halo_kernel, n_sp),
        out_shape=(
            jax.ShapeDtypeStruct((n_sp,) + meta.shape, meta.dtype),
            jax.ShapeDtypeStruct(edges.shape, edges.dtype),
        ),
        in_specs=[VMEM, VMEM],
        out_specs=(VMEM, VMEM),
        scratch_shapes=[
            pltpu.SemaphoreType.DMA((n_sp - 1,)),
            pltpu.SemaphoreType.DMA((n_sp - 1,)),
            pltpu.SemaphoreType.DMA((2,)),
            pltpu.SemaphoreType.DMA((2,)),
        ],
        compiler_params=pltpu.CompilerParams(collective_id=0, has_side_effects=True),
        name="halo",
    )(meta, edges)


def exchange_kernel(count, pieces, place, parts_ref, out_ref, send_sem, recv_sem):
    me, peer_at = place()
    greet([peer_at(lax.rem(me + d, count)) for d in range(1, count)])
    copies = []
    for piece in range(pieces):
        for d in range(1, count):
            there = lax.rem(me + d, count)
            copies.append(
                remote(
                    parts_ref.at[there, piece],
                    out_ref.at[d - 1, piece],
                    send_sem.at[d - 1, piece],
                    recv_sem.at[d - 1, piece],
                    peer_at(there),
                )
            )
    for copy in copies:
        copy.start()
    for copy in copies:
        copy.wait()


def exchange(parts, count, place, collective_id, name):
    pieces = parts.shape[1]
    return pl.pallas_call(
        functools.partial(exchange_kernel, count, pieces, place),
        out_shape=jax.ShapeDtypeStruct((count - 1,) + parts.shape[1:], parts.dtype),
        in_specs=[ANY],
        out_specs=ANY,
        scratch_shapes=[
            pltpu.SemaphoreType.DMA((count - 1, pieces)),
            pltpu.SemaphoreType.DMA((count - 1, pieces)),
        ],
        compiler_params=pltpu.CompilerParams(
            collective_id=collective_id, has_side_effects=True
        ),
        name=name,
    )(parts)


def world_kernel(grid, own_ref, out_ref, send_sem, recv_sem, own_sem):
    nz, nx, ny, nc = grid
    sp, tp = lax.axis_index("sp"), lax.axis_index("tp")
    z, x, y, c = sp // nx, lax.rem(sp, nx), tp // nc, lax.rem(tp, nc)
    half = own_ref.shape[1] // 2

    def device(dz, dx, dy, dc):
        at_z, at_x = lax.rem(z + dz, nz), lax.rem(x + dx, nx)
        at_y, at_c = lax.rem(y + dy, ny), lax.rem(c + dc, nc)
        return at_z * nx + at_x, at_y * nc + at_c

    z_peers = [device(d, 0, 0, 0) for d in range(1, nz)]
    x_peers = [device(0, d, 0, 0) for d in range(1, nx)]
    y_peers = [device(0, 0, d, 0) for d in range(1, ny)]
    c_peers = [device(0, 0, 0, d) for d in range(1, nc)]
    greet(z_peers + x_peers + y_peers + c_peers)
    sent = []

    def block_of(place):
        at_sp, at_tp = device(*place)
        return at_sp * (ny * nc) + at_tp

    def view(place, h):
        return out_ref.at[block_of(place), :, pl.ds(h * half, half)]

    def push(place, h, peers):
        own = place == (0, 0, 0, 0)
        src = own_ref.at[:, pl.ds(h * half, half)] if own else view(place, h)
        for peer in peers:
            copy = remote(
                src,
                view(place, h),
                send_sem.at[len(sent)],
                recv_sem.at[block_of(place), h],
                peer,
            )
            copy.start()
            sent.append(copy)

    def arrived(place, h):
        remote(
            view(place, h),
            view(place, h),
            send_sem.at[0],
            recv_sem.at[block_of(place), h],
            (sp, tp),
        ).wait_recv()

    mine = (0, 0, 0, 0)
    keep = pltpu.make_async_copy(own_ref, out_ref.at[block_of(mine)], own_sem)
    for peer in z_peers:
        for h in range(2):
            push(mine, h, [peer])
    first, second = (x_peers, y_peers), (y_peers, x_peers)
    for h in range(2):
        push(mine, h, first[h])
        push(mine, h, second[h])
        push(mine, h, c_peers)
    keep.start()

    def level_one(dz):
        for h in range(2):
            if dz > 0:
                arrived((dz, 0, 0, 0), h)
                push((dz, 0, 0, 0), h, first[h])
                push((dz, 0, 0, 0), h, second[h])
                push((dz, 0, 0, 0), h, c_peers)

    def level_two(dz):
        for h in range(2):
            for d in range(1, (nx, ny)[h]):
                place = (dz, d, 0, 0) if h == 0 else (dz, 0, d, 0)
                arrived(place, h)
                push(place, h, second[h])
                push(place, h, c_peers)

    def level_three(dz):
        for h in range(2):
            for da in range((nx, ny)[h]):
                for db in range(1, (ny, nx)[h]):
                    place = (dz, da, db, 0) if h == 0 else (dz, db, da, 0)
                    arrived(place, h)
                    push(place, h, c_peers)

    for step in range(nz + 1):
        if step < nz:
            level_one(step)
            level_two(step)
        if step > 0:
            level_three(step - 1)
    for dz in range(nz):
        for dx in range(nx):
            for dy in range(ny):
                for dc in range(1, nc):
                    for h in range(2):
                        arrived((dz, dx, dy, dc), h)
    for copy in sent:
        copy.wait_send()
    keep.wait()


def gather_world(own, n_sp, n_tp):
    grid = grid_of(n_sp, n_tp)
    blocks = n_sp * n_tp
    return pl.pallas_call(
        functools.partial(world_kernel, grid),
        out_shape=jax.ShapeDtypeStruct((blocks,) + own.shape, own.dtype),
        in_specs=[VMEM],
        out_specs=ANY,
        scratch_shapes=[
            pltpu.SemaphoreType.DMA((2 * blocks,)),
            pltpu.SemaphoreType.DMA((blocks, 2)),
            pltpu.SemaphoreType.DMA,
        ],
        compiler_params=pltpu.CompilerParams(collective_id=1, has_side_effects=True),
        name="world",
    )(own)


def columns_kernel(ny, nc, pieces, own_ref, out_ref, send_sem, recv_sem, own_sem):
    sp, tp = lax.axis_index("sp"), lax.axis_index("tp")
    y, c = tp // nc, lax.rem(tp, nc)
    rows, width = own_ref.shape
    step = rows // pieces

    def member(dy, dc):
        return lax.rem(y + dy, ny) * nc + lax.rem(c + dc, nc)

    y_peers = [(sp, member(d, 0)) for d in range(1, ny)]
    c_peers = [(sp, member(0, d)) for d in range(1, nc)]
    greet(y_peers + c_peers)
    sent = []

    def view(dy, dc, piece):
        start = pl.multiple_of(member(dy, dc) * width, width)
        return out_ref.at[pl.ds(piece * step, step), pl.ds(start, width)]

    def push(dy, piece, peers):
        src = own_ref.at[pl.ds(piece * step, step)] if dy == 0 else view(dy, 0, piece)
        for peer in peers:
            copy = remote(
                src,
                view(dy, 0, piece),
                send_sem.at[len(sent)],
                recv_sem.at[member(dy, 0), piece],
                peer,
            )
            copy.start()
            sent.append(copy)

    def arrived(dy, dc, piece):
        ref = view(dy, dc, piece)
        remote(
            ref, ref, send_sem.at[0], recv_sem.at[member(dy, dc), piece], (sp, tp)
        ).wait_recv()

    start = pl.multiple_of(tp * width, width)
    keep = pltpu.make_async_copy(own_ref, out_ref.at[:, pl.ds(start, width)], own_sem)
    keep.start()
    for piece in range(pieces):
        push(0, piece, y_peers)
    for piece in range(pieces):
        push(0, piece, c_peers)
    for piece in range(pieces):
        for dy in range(1, ny):
            arrived(dy, 0, piece)
            push(dy, piece, c_peers)
    for piece in range(pieces):
        for dy in range(ny):
            for dc in range(1, nc):
                arrived(dy, dc, piece)
    for copy in sent:
        copy.wait_send()
    keep.wait()


def gather_columns(own, n_sp, n_tp):
    rows, width = own.shape
    if width % 128 or n_sp * n_tp > MOST_BLOCKS:
        return lax.all_gather(own, "tp", axis=1, tiled=True)
    _, _, ny, nc = grid_of(n_sp, n_tp)
    pieces = 9 if rows % (9 * 16) == 0 else 1
    return pl.pallas_call(
        functools.partial(columns_kernel, ny, nc, pieces),
        out_shape=jax.ShapeDtypeStruct((rows, n_tp * width), own.dtype),
        in_specs=[VMEM],
        out_specs=ANY,
        scratch_shapes=[
            pltpu.SemaphoreType.DMA((n_tp * pieces,)),
            pltpu.SemaphoreType.DMA((n_tp, pieces)),
            pltpu.SemaphoreType.DMA,
        ],
        compiler_params=pltpu.CompilerParams(collective_id=2, has_side_effects=True),
        name="columns",
    )(own)


def rows_kernel(grid, cuts, parts_ref, columns_ref, own_ref, from_z_ref, residual_ref, from_x, staged, x_send, x_recv, z_send, z_recv, tp_send, tp_recv):
    nz, nx, ny, nc = grid
    n_tp = ny * nc
    sp, tp = lax.axis_index("sp"), lax.axis_index("tp")
    z, x = sp // nx, lax.rem(sp, nx)
    x_peers = [(z * nx + lax.rem(x + d, nx), tp) for d in range(1, nx)]
    z_peers = [(lax.rem(z + d, nz) * nx + x, tp) for d in range(1, nz)]
    tp_peers = [(sp, lax.rem(tp + d, n_tp)) for d in range(1, n_tp)]
    greet(x_peers + z_peers + tp_peers)
    step = parts_ref.shape[2] // cuts
    turns = [(dz, cut) for dz in list(range(1, nz)) + [0] for cut in range(cuts)]
    x_copies, others = {}, []
    for dz, cut in turns:
        rows = pl.ds(cut * step, step)
        for d in range(1, nx):
            copy = remote(
                parts_ref.at[lax.rem(z + dz, nz), lax.rem(x + d, nx), rows],
                from_x.at[d - 1, dz, rows],
                x_send.at[d - 1, dz, cut],
                x_recv.at[d - 1, dz, cut],
                x_peers[d - 1],
            )
            copy.start()
            x_copies[d, dz, cut] = copy
    for d in range(1, n_tp):
        copy = remote(
            columns_ref.at[lax.rem(tp + d, n_tp)],
            residual_ref.at[tp],
            tp_send.at[d - 1],
            tp_recv.at[d - 1],
            tp_peers[d - 1],
        )
        copy.start()
        others.append(copy)
    residual_ref[tp] = columns_ref[tp]
    for dz, cut in turns:
        rows = pl.ds(cut * step, step)
        total = parts_ref[lax.rem(z + dz, nz), x, rows].astype(jnp.float32)
        for d in range(1, nx):
            x_copies[d, dz, cut].wait_recv()
            total = total + from_x[d - 1, dz, rows].astype(jnp.float32)
        if dz == 0:
            own_ref[rows] = total
            continue
        staged[dz - 1, rows] = total.astype(staged.dtype)
        copy = remote(
            staged.at[dz - 1, rows],
            from_z_ref.at[dz - 1, rows],
            z_send.at[dz - 1, cut],
            z_recv.at[dz - 1, cut],
            z_peers[dz - 1],
        )
        copy.start()
        others.append(copy)
    for copy in x_copies.values():
        copy.wait_send()
    for copy in others:
        copy.wait()


def sum_rows(parts, columns, n_sp, n_tp):
    grid = grid_of(n_sp, n_tp)
    nz, nx, _, _ = grid
    tok_dev, d_dev = parts.shape[2:]
    cuts = 2
    return pl.pallas_call(
        functools.partial(rows_kernel, grid, cuts),
        out_shape=(
            jax.ShapeDtypeStruct((tok_dev, d_dev), jnp.float32),
            jax.ShapeDtypeStruct((nz - 1, tok_dev, d_dev), parts.dtype),
            jax.ShapeDtypeStruct(columns.shape, columns.dtype),
        ),
        in_specs=[VMEM, VMEM],
        out_specs=(VMEM, VMEM, VMEM),
        scratch_shapes=[
            pltpu.VMEM((nx - 1, nz, tok_dev, d_dev), parts.dtype),
            pltpu.VMEM((nz - 1, tok_dev, d_dev), parts.dtype),
            pltpu.SemaphoreType.DMA((nx - 1, nz, cuts)),
            pltpu.SemaphoreType.DMA((nx - 1, nz, cuts)),
            pltpu.SemaphoreType.DMA((nz - 1, cuts)),
            pltpu.SemaphoreType.DMA((nz - 1, cuts)),
            pltpu.SemaphoreType.DMA((n_tp - 1,)),
            pltpu.SemaphoreType.DMA((n_tp - 1,)),
        ],
        compiler_params=pltpu.CompilerParams(collective_id=4, has_side_effects=True),
        name="rows",
    )(parts, columns)


def attention(queries, band, sink, sp_idx, n_sp):
    tok_dev = queries.shape[0]
    blocks = tok_dev // WINDOW
    heads_dev = queries.shape[1] // HD
    framed = band.reshape(blocks + 2, WINDOW, 2 * HD)
    banded = jnp.concatenate([framed[:-2], framed[1:-1], framed[2:]], axis=1)
    key_band = banded[:, :, :HD]
    value_band = banded[:, :, HD:]
    query_blocks = queries.reshape(blocks, WINDOW, heads_dev, HD)
    scores = jnp.einsum(
        "nqhd,njd->nhqj", query_blocks, key_band, preferred_element_type=jnp.float32
    ) * HD ** (-0.5)
    offset = sp_idx * tok_dev
    seq_total = tok_dev * n_sp
    query_pos = (
        offset + jnp.arange(blocks)[:, None, None] * WINDOW + jnp.arange(WINDOW)[None, :, None]
    )
    key_pos = (
        offset
        - WINDOW
        + jnp.arange(blocks)[:, None, None] * WINDOW
        + jnp.arange(3 * WINDOW)[None, None, :]
    )
    allowed = (jnp.abs(query_pos - key_pos) <= WINDOW) & (key_pos >= 0) & (key_pos < seq_total)
    scores = jnp.where(allowed[:, None], scores, -jnp.inf)
    sink_level = sink.reshape(1, heads_dev, 1, 1)
    row_peak = jnp.maximum(scores.max(-1, keepdims=True), sink_level)
    probabilities = jnp.exp(scores - row_peak)
    denominator = probabilities.sum(-1, keepdims=True) + jnp.exp(sink_level - row_peak)
    weights = (probabilities / denominator).astype(jnp.bfloat16)
    attended = jnp.einsum("nhqj,njd->nqhd", weights, value_band, preferred_element_type=jnp.float32)
    return attended.astype(jnp.bfloat16).reshape(tok_dev, heads_dev * HD)


def norm(rows, gain):
    wide = rows.astype(jnp.float32)
    scale = lax.rsqrt(jnp.mean(wide * wide, axis=-1, keepdims=True) + NORM_EPS)
    return (wide * scale * gain.astype(jnp.float32)).astype(jnp.bfloat16)


def local(
    queries,
    keys,
    values,
    sink,
    w_out,
    stream,
    gain,
    routes,
    route_weights,
    w_gate,
    w_up,
    w_down,
    shared_gate,
    shared_up,
    shared_down,
):
    tok_dev = queries.shape[0]
    n_tp = lax.axis_size("tp")
    n_sp = lax.axis_size("sp")
    tp_idx = lax.axis_index("tp")
    sp_idx = lax.axis_index("sp")
    nz, nx, _, _ = grid_of(n_sp, n_tp)
    heads_dev = HEADS // n_tp
    group = HEADS // KV_HEADS
    kv_head = tp_idx * heads_dev // group
    key_own = lax.dynamic_slice_in_dim(keys, kv_head * HD, HD, 1)
    value_own = lax.dynamic_slice_in_dim(values, kv_head * HD, HD, 1)
    paired = jnp.concatenate([key_own, value_own], axis=1)
    edges = jnp.stack([paired[-WINDOW:], paired[:WINDOW]])
    meta = jnp.concatenate([routes.astype(jnp.float32).T, route_weights.T], axis=0)
    metas, halo = exchange_halo(meta, edges, n_sp)
    band = jnp.concatenate([halo[0], paired, halo[1]], axis=0)
    attended = attention(queries, band, sink, sp_idx, n_sp)
    rows_dev = tok_dev // n_tp
    d_dev = w_down.shape[2]

    partial = jnp.dot(attended, w_out, preferred_element_type=jnp.float32)
    parts = partial.astype(jnp.bfloat16).reshape(n_tp, 1, rows_dev, D)
    theirs = exchange(
        parts,
        n_tp,
        lambda: (lax.axis_index("tp"), lambda there: (lax.axis_index("sp"), there)),
        3,
        "heads",
    )
    own_part = lax.dynamic_slice_in_dim(partial, tp_idx * rows_dev, rows_dev, 0)
    projected = own_part + jnp.sum(theirs[:, 0].astype(jnp.float32), axis=0)
    mixed_rows = (stream.astype(jnp.float32) + projected).astype(jnp.bfloat16)
    own_norm = norm(mixed_rows, gain)
    if n_sp * n_tp > MOST_BLOCKS:
        normed = lax.all_gather(own_norm, ("sp", "tp"), axis=0)
    else:
        normed = gather_world(own_norm, n_sp, n_tp)
    own_normed = lax.dynamic_slice_in_dim(normed, sp_idx * n_tp, n_tp, 0).reshape(tok_dev, D)

    exp_dev = w_gate.shape[0]
    capacity = max(1, 2 * tok_dev * TOPK // (n_tp * EXPERTS))
    n_blocks = n_sp * n_tp
    order = lax.rem(sp_idx - jnp.arange(n_sp) + n_sp, n_sp)
    pick = (order[None, :] == jnp.arange(n_sp)[:, None]).astype(jnp.float32)
    metas = jnp.sum(pick[:, :, None, None] * metas[None], axis=1)
    metas = metas.reshape(n_sp, 2, TOPK, n_tp, rows_dev).transpose(1, 0, 3, 2, 4)
    named = metas[0].reshape(n_blocks, 1, TOPK, rows_dev)
    weight = metas[1].reshape(n_blocks, 1, TOPK, rows_dev)
    experts = (sp_idx * exp_dev + jnp.arange(exp_dev)).astype(jnp.float32)
    hit = (named == experts[None, :, None, None]).astype(jnp.float32)
    hit_any = jnp.sum(hit, axis=2)
    hit_weight = jnp.sum(hit * weight, axis=2)
    earlier = (jnp.arange(rows_dev)[:, None] < jnp.arange(rows_dev)[None, :]).astype(jnp.bfloat16)
    rank = jnp.einsum(
        "bej,jr->ber", hit_any.astype(jnp.bfloat16), earlier, preferred_element_type=jnp.float32
    )
    slots = jnp.arange(capacity).astype(jnp.float32)
    select = (rank[:, :, None, :] == slots[None, None, :, None]) * hit_any[:, :, None, :]
    slot_weight = jnp.sum(select * hit_weight[:, :, None, :], axis=-1)
    table = select.astype(jnp.bfloat16)

    arrived = jnp.einsum(
        "becr,brd->ebcd", table, normed, preferred_element_type=jnp.float32
    ).astype(jnp.bfloat16)
    arrived = arrived.reshape(exp_dev, n_blocks * capacity, D)
    gate_act = jnp.einsum("emd,efd->emf", arrived, w_gate, preferred_element_type=jnp.float32)
    up_act = jnp.einsum("emd,efd->emf", arrived, w_up, preferred_element_type=jnp.float32)
    hidden = (jax.nn.silu(gate_act) * up_act).astype(jnp.bfloat16)
    shared_gate_act = jnp.einsum(
        "td,fd->tf", own_normed, shared_gate, preferred_element_type=jnp.float32
    )
    shared_up_act = jnp.einsum(
        "td,fd->tf", own_normed, shared_up, preferred_element_type=jnp.float32
    )
    shared_hidden = (jax.nn.silu(shared_gate_act) * shared_up_act).astype(jnp.bfloat16)
    routed_rows = exp_dev * n_blocks * capacity
    width = hidden.shape[2]
    both = jnp.concatenate([hidden.reshape(routed_rows, width), shared_hidden], axis=0)
    both = gather_columns(both, n_sp, n_tp)
    expert_piece = both[:routed_rows].reshape(exp_dev, n_blocks * capacity, n_tp * width)
    routed_out = jnp.einsum(
        "emf,efd->emd", expert_piece, w_down, preferred_element_type=jnp.float32
    )
    scaled = routed_out.reshape(exp_dev, n_blocks, capacity, d_dev)
    scaled = scaled * slot_weight.transpose(1, 0, 2)[..., None]
    scaled = scaled.astype(jnp.bfloat16)
    sums = jnp.einsum("becr,ebcd->brd", table, scaled, preferred_element_type=jnp.float32)
    sums = sums.astype(jnp.bfloat16).reshape(nz, nx, tok_dev, d_dev)
    columns = mixed_rows.reshape(rows_dev, n_tp, d_dev).transpose(1, 0, 2)
    own_sum, from_z, residual = sum_rows(sums, columns, n_sp, n_tp)
    residual = residual.reshape(tok_dev, d_dev).astype(jnp.float32)
    routed = own_sum + jnp.sum(from_z.astype(jnp.float32), axis=0)
    shared_total = jnp.dot(both[routed_rows:], shared_down, preferred_element_type=jnp.float32)
    return (residual + routed + shared_total).astype(jnp.bfloat16)


def solution(mesh):
    placed = (
        P("sp", "tp"),
        P("sp", None),
        P("sp", None),
        P("tp"),
        P("tp", None),
        P(("sp", "tp"), None),
        P(),
        P("sp", None),
        P("sp", None),
        P("sp", "tp", None),
        P("sp", "tp", None),
        P("sp", None, "tp"),
        P("tp", None),
        P("tp", None),
        P(None, "tp"),
    )
    return jax.shard_map(
        local, mesh=mesh, in_specs=placed, out_specs=P("sp", "tp"), check_vma=False
    )
```
